32 devices in a mesh: grp: 2 (over y), ep: 4 (over z), tp: 4 (over x, core).
Axes of the slice: x: 2, y: 2, z: 4, core: 2. Of those that a mesh axis runs over, the one named last changes fastest.
Arguments:
- tokens: bfloat16 [3072, 2048], P(('grp', 'ep'), 'tp'), parts along dimension 0
- group_choice: int32 [3072], P(('grp', 'ep')), parts along dimension 0, may hold values from 0 to 1, as said below
- expert_choice: int32 [3072, 2], P(('grp', 'ep')), parts along dimension 0, may hold values from 0 to 1, as said below
- group_weight: float32 [3072], P(('grp', 'ep')), parts along dimension 0, may hold values from 0.3 to 1
- expert_weight: float32 [3072, 2], P(('grp', 'ep')), parts along dimension 0, may hold values from 0.1 to 1
- norm_gain: float32 [2048], replicated, may hold values from 0.1 to 1.9
- w_gate: bfloat16 [4, 2048, 1024], P('ep', None, 'tp'), may hold values from -0.125 to 0.125
- w_up: bfloat16 [4, 2048, 1024], P('ep', None, 'tp'), may hold values from -0.125 to 0.125
- w_down: bfloat16 [4, 1024, 2048], P('ep', None, 'tp'), may hold values from -0.1875 to 0.1875
Outputs:
- moe_out: bfloat16 [3072, 2048], P(('grp', 'ep'), 'tp'), parts along dimension 0
The draws below stay inside these ranges and needn't reach their ends.
There are 2 independent parts, one for each index of `grp`. The reference program is written for one: setup_inputs(seed, part) draws one part's arguments, and reference() takes and returns one part's arrays. A program takes and returns all parts, laid end to end along the dimension named above; an argument that names none is the same for every part. Nothing has to cross between parts.
Inputs may be any that keep to these rules, and one draw needn't show every extreme that they name: `group_choice`: group of each token, 0 to 1; within each aligned block of 384 tokens (the tokens of one index of ep) every group is chosen by the same number of tokens. `expert_choice`: a token's two entries differ; within each aligned block of 384 tokens no expert (group with entry) is named by more than 192 tokens, and in every block one expert of each group, the same one in all blocks, is named by exactly 192 tokens.
All inputs are finite; a program needn't handle non-finite values.
Results may differ from the reference program's by a relative error of at most 0.0071.
Values may be sent and summed in bfloat16 or wider, within the bound.
A program may use at most 64 MiB of HBM per device.

```python
import math
import jax
import jax.numpy as jnp
from jax import lax

D = 2048
FF = 1024
TOK_DEV = 384
TOP_K = 2
EXPERTS = 4
EXPERTS_GROUP = 2
GROUPS = 2
CAP = 192
TOKENS = 1536


def route_tables(key):
    base = jax.random.fold_in(key, 11)
    per_group = TOK_DEV // GROUPS
    mean_load = 2 * per_group // EXPERTS_GROUP
    swing = min(mean_load // 2, per_group - mean_load)
    pairs = EXPERTS_GROUP // 2
    blocks = TOKENS // TOK_DEV
    order_keys = jax.random.split(jax.random.fold_in(base, 1), GROUPS)
    orders = jax.vmap(lambda one_key: jax.random.permutation(one_key, EXPERTS_GROUP))(order_keys)

    def one_block(block_key):
        key_shift, key_seat, key_flip = jax.random.split(block_key, 3)
        shifts = jax.random.randint(key_shift, (GROUPS, pairs), -swing, swing + 1)
        shifts = shifts.at[:, 0].set(swing)
        loads = jnp.stack([mean_load + shifts, mean_load - shifts], -1).reshape(GROUPS, EXPERTS_GROUP)
        placed = jnp.zeros((GROUPS, EXPERTS_GROUP), jnp.int32).at[jnp.arange(GROUPS)[:, None], orders].set(loads.astype(jnp.int32))
        ends = jnp.cumsum(placed, -1)
        spots = jnp.arange(2 * per_group, dtype=jnp.int32)
        labels = jnp.sum((spots[None, :, None] >= ends[:, None, :]).astype(jnp.int32), -1)
        first = labels[:, :per_group].reshape(-1)
        second = labels[:, per_group:].reshape(-1)
        flips = jax.random.randint(key_flip, (TOK_DEV,), 0, 2)
        first_swapped = jnp.where(flips == 1, second, first)
        second_swapped = jnp.where(flips == 1, first, second)
        seats = jax.random.permutation(key_seat, TOK_DEV)
        group_rank = (jnp.arange(TOK_DEV, dtype=jnp.int32) // per_group).astype(jnp.int32)
        group_of = jnp.zeros((TOK_DEV,), jnp.int32).at[seats].set(group_rank)
        first_of = jnp.zeros((TOK_DEV,), jnp.int32).at[seats].set(first_swapped)
        second_of = jnp.zeros((TOK_DEV,), jnp.int32).at[seats].set(second_swapped)
        return (group_of, jnp.stack([first_of, second_of], -1))
    block_keys = jax.random.split(jax.random.fold_in(base, 2), blocks)
    groups_all, experts_all = jax.vmap(one_block)(block_keys)
    return (groups_all.reshape(TOKENS), experts_all.reshape(TOKENS, TOP_K))


def draw_group_choice(key, part):
    return route_tables(key)[0]


def draw_expert_choice(key, part):
    return route_tables(key)[1]


def draw_tokens(key, part):
    key_main = jax.random.fold_in(jax.random.fold_in(key, 5), 0)
    column_scale = jnp.exp(math.log(4.0) * jnp.arange(D, dtype=jnp.float32) / D)
    values = jax.random.normal(key_main, (TOKENS, D), jnp.float32)
    return (values * column_scale[None, :]).astype(jnp.bfloat16)


def shard_levels(rng, shape, pieces, low, top_value):
    gain = 1.0
    for axis_at, parts in pieces:
        steps = jax.random.uniform(jax.random.fold_in(jax.random.fold_in(rng, 6), axis_at), (parts,), jnp.float32, low / len(pieces), top_value / len(pieces))
        gain = gain * jnp.repeat(jnp.exp(steps), shape[axis_at] // parts).reshape((-1,) + (1,) * (len(shape) - 1 - axis_at))
    return gain


def bell_draw(own_key, shape, deviation, most, cuts=(), held_as=jnp.bfloat16):
    values = deviation * jax.random.normal(own_key, shape, jnp.float32)
    if cuts:
        values = values * shard_levels(own_key, shape, cuts, -0.22, 0.18)
    return jnp.clip(values, -most, most).astype(held_as)


def setup_inputs(seed: int = 0, part: int = 0) -> dict:
    key_list = jax.random.split(jax.random.key(seed), 10)
    part_splits = jax.random.split(jax.random.fold_in(key_list[9], part), 10)
    return {
        "tokens": draw_tokens(jax.random.fold_in(jax.random.fold_in(key_list[9], part), 71), part),
        "group_choice": draw_group_choice(jax.random.fold_in(jax.random.fold_in(key_list[9], part), 71), part),
        "expert_choice": draw_expert_choice(jax.random.fold_in(jax.random.fold_in(key_list[9], part), 71), part),
        "group_weight": jnp.clip(0.3 + 0.7 * jax.random.uniform(part_splits[3], (TOKENS,), jnp.float32) ** shard_levels(part_splits[3], (TOKENS,), ((0, 4),), -0.2, 0.2), 0.3, 1.0),
        "expert_weight": jnp.clip(jnp.exp(math.log(1.0) - 2.3025851 * jax.random.uniform(part_splits[4], (TOKENS, TOP_K), jnp.float32) ** shard_levels(part_splits[4], (TOKENS, TOP_K), ((0, 4),), -0.2, 0.2)), 0.1, 1.0),
        "norm_gain": jnp.clip(1.0 + 0.18 * jax.random.normal(key_list[5], (D,), jnp.float32), 0.1, 1.9),
        "w_gate": bell_draw(key_list[6], (EXPERTS, D, FF), D ** -0.5, 0.125, ((0, 4), (2, 4))),
        "w_up": bell_draw(key_list[7], (EXPERTS, D, FF), D ** -0.5, 0.125, ((0, 4), (2, 4))),
        "w_down": bell_draw(key_list[8], (EXPERTS, FF, D), FF ** -0.5, 0.1875, ((0, 4), (2, 4))),
    }


def reference(tokens, group_choice, expert_choice, group_weight, expert_weight, norm_gain, w_gate, w_up, w_down):
    values = tokens.astype(jnp.float32)
    inv_rms = lax.rsqrt(lax.optimization_barrier(jnp.mean(values * values, -1, keepdims=True)) + 1e-06)
    normed = (values * inv_rms * norm_gain.astype(jnp.float32)).astype(jnp.bfloat16)
    expert_ids = (group_choice[:, None] * EXPERTS_GROUP + expert_choice).astype(jnp.int32)
    mixing = group_weight[:, None] * expert_weight / lax.optimization_barrier(jnp.sum(expert_weight, -1, keepdims=True))
    flat_ids = expert_ids.reshape(-1)
    flat_tokens = jnp.repeat(jnp.arange(TOKENS, dtype=jnp.int32), TOP_K)
    flat_mix = mixing.reshape(-1)
    ordering = jnp.argsort(flat_ids, stable=True).astype(jnp.int32)
    sorted_tokens = flat_tokens[ordering]
    sorted_mix = flat_mix[ordering]
    counts = lax.optimization_barrier(jnp.sum((flat_ids[None, :] == jnp.arange(EXPERTS, dtype=jnp.int32)[:, None]).astype(jnp.int32), 1))
    starts = jnp.cumsum(counts) - counts
    rows_most = TOKENS // TOK_DEV * CAP
    offsets = jnp.arange(rows_most, dtype=jnp.int32)

    def per_expert(summed, expert):
        places = jnp.minimum(starts[expert] + offsets, TOKENS * TOP_K - 1).astype(jnp.int32)
        alive = offsets < counts[expert]
        token_rows = sorted_tokens[places]
        weights = jnp.where(alive, sorted_mix[places], 0.0)
        chosen = normed[token_rows]
        gate_sum = jnp.dot(chosen, w_gate[expert], preferred_element_type=jnp.float32)
        up_sum = jnp.dot(chosen, w_up[expert], preferred_element_type=jnp.float32)
        hidden = (jax.nn.silu(gate_sum) * up_sum).astype(jnp.bfloat16)
        result = jnp.dot(hidden, w_down[expert], preferred_element_type=jnp.float32).astype(jnp.bfloat16)
        summed = summed.at[token_rows].add(result.astype(jnp.float32) * weights[:, None])
        return (summed, None)
    initial = jnp.zeros((TOKENS, D), jnp.float32)
    summed, _ = lax.scan(per_expert, initial, jnp.arange(EXPERTS, dtype=jnp.int32))
    return summed.astype(jnp.bfloat16)
```

```python
import functools

import jax
import jax.numpy as jnp
from jax import lax
from jax.experimental import pallas as pl
from jax.experimental.pallas import tpu as pltpu
from jax.sharding import PartitionSpec as P

MESH = pl.DeviceIdType.MESH


def finish_rows(gate_sum, up_sum, w_down):
    hidden = (jax.nn.silu(gate_sum) * up_sum).astype(jnp.bfloat16)
    whole_hidden = lax.all_gather(hidden, "tp", axis=3, tiled=True)
    summed = jnp.einsum("sxcf,xfd->sxcd", whole_hidden, w_down, preferred_element_type=jnp.float32)
    return summed.astype(jnp.bfloat16)


def body(
    tokens,
    group_choice,
    expert_choice,
    group_weight,
    expert_weight,
    norm_gain,
    w_gate,
    w_up,
    w_down,
):
    tok_rows = tokens.shape[0]
    ep_count = lax.axis_size("ep")
    exp_local = w_gate.shape[0]
    experts_all = ep_count * exp_local
    group_size = min(8, experts_all // 2)
    group_count = experts_all // group_size
    mean_load = 2 * tok_rows // experts_all
    capacity = mean_load + min(mean_load // 2, tok_rows // group_count - mean_load)
    model_width = norm_gain.shape[0]
    expert_ids = group_choice[:, None] * group_size + expert_choice
    mixing = group_weight[:, None] * expert_weight / jnp.sum(expert_weight, -1, keepdims=True)
    flat_ids = expert_ids.reshape(-1)
    marks = (flat_ids[:, None] == jnp.arange(experts_all, dtype=jnp.int32)[None, :]).astype(
        jnp.int32
    )
    earlier = jnp.cumsum(marks, 0) - marks
    seat_index = jnp.sum(earlier * marks, 1)
    targets = (flat_ids * capacity + seat_index).reshape(tok_rows, 2)
    places = jnp.arange(experts_all * capacity, dtype=jnp.int32)
    dispatch = (
        (places[:, None] == targets[None, :, 0]) | (places[:, None] == targets[None, :, 1])
    ).astype(jnp.bfloat16)
    values = tokens.astype(jnp.float32)
    own_squares = jnp.sum(values * values, -1)
    all_squares = lax.psum(own_squares, "tp")
    inv_rms = lax.rsqrt(all_squares / model_width + 1e-06)
    piece_width = tokens.shape[1]
    gain_piece = lax.dynamic_slice_in_dim(
        norm_gain, lax.axis_index("tp") * piece_width, piece_width, 0
    )
    normed = (values * inv_rms[:, None] * gain_piece[None, :]).astype(jnp.bfloat16)
    buffer = jnp.dot(dispatch, normed, preferred_element_type=jnp.float32).astype(jnp.bfloat16)
    buffer = buffer.reshape(ep_count, exp_local, capacity, piece_width)
    piece = lax.all_gather(
        lax.all_to_all(buffer, "ep", split_axis=0, concat_axis=0, tiled=True),
        "tp",
        axis=3,
        tiled=True,
    )
    gate_next = jnp.einsum("sxcd,xdf->sxcf", piece, w_gate, preferred_element_type=jnp.float32)
    up_next = jnp.einsum("sxcd,xdf->sxcf", piece, w_up, preferred_element_type=jnp.float32)
    results = finish_rows(gate_next, up_next, w_down)
    returned = lax.all_to_all(results, "ep", split_axis=0, concat_axis=0, tiled=True)
    returned = returned.reshape(experts_all * capacity, returned.shape[3])
    combined = jnp.zeros((tok_rows, returned.shape[1]), jnp.float32)
    for choice_index in range(2):
        picker = (targets[:, choice_index : choice_index + 1] == places[None, :]).astype(
            jnp.bfloat16
        )
        picked = jnp.dot(picker, returned, preferred_element_type=jnp.float32)
        combined = combined + mixing[:, choice_index : choice_index + 1] * picked
    return combined.astype(jnp.bfloat16)


def layer_kernel(
    chunks,
    group_hbm,
    choice_hbm,
    group_weight_hbm,
    expert_weight_hbm,
    gain_hbm,
    tok_hbm,
    gate_hbm,
    up_hbm,
    down_hbm,
    out_ref,
    group_ref,
    choice_ref,
    group_weight_ref,
    expert_weight_ref,
    gain_ref,
    tok_ref,
    w_gate,
    w_up,
    w_down,
    rows,
    other,
    hid,
    outs,
    back,
    home,
    place,
    comb,
    mix_rows,
    mix_far,
    norm,
    wsem,
    z_send,
    z_recv,
    fwd_send,
    x_send,
    x_recv,
    h_send,
    h_recv,
    r_send,
    r_recv,
    c_send,
    c_recv,
    m_send,
    m_recv,
):
    z = lax.axis_index("ep")
    t = lax.axis_index("tp")
    group = z // 2
    parity = z % 2
    inner = (parity + group) % 2
    is_inner = inner == 1
    is_outer = inner == 0
    partner = z + 1 - 2 * parity
    cross = 2 - group
    cross_outer = 3 * (1 - group)
    near = t + 1 - 2 * (t % 2)
    far = (t + 2) % 4
    diag = (near + 2) % 4
    size, width = rows.shape[2:]
    half = size * chunks
    count = 2 * half
    items = 4 * chunks
    model_width = 4 * width
    hidden_width = hid.shape[3]

    pairs = (
        (gate_hbm, w_gate),
        (up_hbm, w_up),
        (down_hbm, w_down),
        (tok_hbm, tok_ref),
        (group_hbm, group_ref),
        (choice_hbm, choice_ref),
        (group_weight_hbm, group_weight_ref),
        (expert_weight_hbm, expert_weight_ref),
        (gain_hbm, gain_ref),
    )
    loads = [
        pltpu.make_async_copy(source, target, wsem.at[i])
        for i, (source, target) in enumerate(pairs)
    ]

    barrier = pltpu.get_barrier_semaphore()

    def greet(**where):
        pl.semaphore_signal(barrier, inc=1, device_id=where, device_id_type=MESH)

    greet(tp=near)
    greet(tp=far)
    greet(ep=partner)
    greet(ep=cross)

    @pl.when(is_inner)
    def _():
        greet(ep=cross_outer)

    for i in (4, 3, 5, 6, 7, 8, 0, 1, 2):
        loads[i].start()

    def remote(source, target, send, recv, **where):
        return pltpu.make_async_remote_copy(
            src_ref=source,
            dst_ref=target,
            send_sem=send,
            recv_sem=recv,
            device_id=where,
            device_id_type=MESH,
        )

    def arrived(ref, sem):
        remote(ref, ref, sem, sem, tp=near).wait_recv()

    line = lax.broadcasted_iota(jnp.int32, (count, count), 0)
    lane = lax.broadcasted_iota(jnp.int32, (count, count), 1)
    eye = line == lane

    def column(row):
        return jnp.sum(jnp.where(eye, row, 0.0), 1, keepdims=True)

    loads[4].wait()
    own_row = jnp.where(group_ref[...].reshape(1, -1) == group, 1.0, 0.0)
    own_rows = jnp.broadcast_to(own_row, (8, count)).astype(jnp.bfloat16)
    earlier = jnp.where(line < lane, 1.0, 0.0).astype(jnp.bfloat16)
    before = jnp.dot(own_rows, earlier, preferred_element_type=jnp.float32)[0:1, :]
    at = lax.broadcasted_iota(jnp.int32, (1, count), 1).astype(jnp.float32)
    seat_row = jnp.where(own_row > 0.5, before, half + at - before)
    seat_ints = seat_row.astype(jnp.int32)

    def sort_half(start, target):
        want = lax.broadcasted_iota(jnp.int32, (half, count), 0) + start
        order = jnp.where(seat_ints == want, 1.0, 0.0).astype(jnp.bfloat16)
        part = jnp.dot(order, tok_ref[...], preferred_element_type=jnp.float32)
        for c in range(chunks):
            target(c, part[c * size : (c + 1) * size].astype(jnp.bfloat16))

    def keep_own(c, value):
        rows[c, t] = value

    def keep_other(c, value):
        other[c] = value

    loads[3].wait()
    sort_half(0, keep_own)

    pl.semaphore_wait(barrier, 4 + inner)

    slot = 3 - inner

    def own_send(c):
        there = chunks + c
        return remote(rows.at[c, t], rows.at[there, t], z_send.at[c], z_recv.at[there], ep=partner)

    def other_send(c):
        there = slot * chunks + c
        return remote(
            other.at[c], rows.at[there, t], z_send.at[chunks + c], z_recv.at[there], ep=cross
        )

    mix_send = remote(mix_rows, mix_far.at[slot - 2], m_send, m_recv.at[slot - 2], ep=cross)

    def spread(buffer, k, send, recv, step):
        mine = buffer.at[k, t]
        if step == 0:
            remote(mine, mine, send.at[k, 1], recv.at[k, 1], tp=far).start()
            remote(mine, mine, send.at[k, 0], recv.at[k, 0], tp=near).start()
        elif step == 1:
            theirs = buffer.at[k, far]
            arrived(theirs, recv.at[k, 1])
            remote(theirs, theirs, send.at[k, 2], recv.at[k, 2], tp=near).start()
        elif step == 2:
            arrived(buffer.at[k, near], recv.at[k, 0])
            arrived(buffer.at[k, diag], recv.at[k, 2])
        else:
            remote(mine, mine, send.at[k, 1], recv.at[k, 1], tp=far).wait_send()
            remote(mine, mine, send.at[k, 0], recv.at[k, 0], tp=near).wait_send()
            theirs = buffer.at[k, far]
            remote(theirs, theirs, send.at[k, 2], recv.at[k, 2], tp=near).wait_send()

    def relay(k):
        sem = fwd_send.at[k - 2 * chunks]
        return remote(rows.at[k, t], rows.at[k, t], sem, z_recv.at[k], ep=partner)

    def stage_a(k):
        if chunks <= k < 2 * chunks:
            arrived(rows.at[k, t], z_recv.at[k])
        if k >= 2 * chunks:
            pl.when(is_outer)(lambda: arrived(rows.at[k, t], z_recv.at[k]))
        spread(rows, k, x_send, x_recv, 0)

    def stage_r(k):
        @pl.when(is_inner)
        def _():
            arrived(rows.at[k, t], z_recv.at[k])
            relay(k).start()

    def stage_b(k):
        spread(rows, k, x_send, x_recv, 1)

    def stage_c(k):
        spread(rows, k, x_send, x_recv, 2)
        squares = jnp.zeros((size, 1), jnp.float32)
        for j in range(4):
            values = rows[k, j].astype(jnp.float32)
            squares = squares + jnp.sum(values * values, 1, keepdims=True)
        inv_rms = lax.rsqrt(squares / model_width + 1e-06)
        for j in range(4):
            cols = slice(j * width, (j + 1) * width)
            values = rows[k, j].astype(jnp.float32)
            norm[:, cols] = (values * inv_rms * gain_ref[0:1, cols]).astype(jnp.bfloat16)
        if k == 0:
            loads[0].wait()
            loads[1].wait()
        gate = jnp.dot(norm[...], w_gate[...], preferred_element_type=jnp.float32)
        up = jnp.dot(norm[...], w_up[...], preferred_element_type=jnp.float32)
        hid[k, t] = (gate / (1.0 + jnp.exp(-gate)) * up).astype(jnp.bfloat16)
        if k >= chunks:
            spread(hid, k, h_send, h_recv, 0)

    def stage_d(k):
        spread(hid, k, h_send, h_recv, 1)

    def back_send(k):
        there = k - chunks if k < 2 * chunks else k
        return remote(outs.at[k], back.at[there], r_send.at[k], r_recv.at[there], ep=partner)

    def stage_e(k):
        spread(hid, k, h_send, h_recv, 2)
        if k == chunks:
            loads[2].wait()
        total = jnp.zeros((size, width), jnp.float32)
        for j in range(4):
            part = w_down[j * hidden_width : (j + 1) * hidden_width, :]
            total = total + jnp.dot(hid[k, j], part, preferred_element_type=jnp.float32)
        outs[k] = total.astype(jnp.bfloat16)
        if chunks <= k < 2 * chunks:
            back_send(k).start()
        if k >= 2 * chunks:
            pl.when(is_outer)(lambda: back_send(k).start())

    def joined(k, mixes, start):
        arrived(back.at[k], r_recv.at[k])
        start = start + (k % chunks) * size
        low = lax.broadcasted_iota(jnp.int32, (size, count), 0) + start
        pick = low == lax.broadcasted_iota(jnp.int32, (size, count), 1)
        even = jnp.sum(jnp.where(pick, mixes[0:1, :], 0.0), 1, keepdims=True)
        odd = jnp.sum(jnp.where(pick, mixes[1:2, :], 0.0), 1, keepdims=True)
        mine = jnp.where(parity == 0, even, odd)
        theirs = jnp.where(parity == 0, odd, even)
        summed = mine * outs[k].astype(jnp.float32) + theirs * back[k].astype(jnp.float32)
        return summed.astype(jnp.bfloat16)

    def comb_send(k):
        where = cross if k < 3 * chunks else cross_outer
        i, c = k - 2 * chunks, k % chunks
        return remote(comb.at[i], home.at[c], c_send.at[i], c_recv.at[c], ep=where)

    def stage_j(k):
        @pl.when(is_inner)
        def _():
            far_slot = k // chunks - 2
            if k % chunks == 0:
                arrived(mix_far.at[far_slot], m_recv.at[far_slot])
            comb[k - 2 * chunks] = joined(k, mix_far[far_slot], half)
            comb_send(k).start()

    stage_a(0)
    for c in range(chunks):
        own_send(c).start()
    sort_half(half, keep_other)
    for c in range(chunks):
        other_send(c).start()
    stage_a(1)
    for i in (5, 6, 7, 8):
        loads[i].wait()
    first, second = expert_weight_ref[0:1, :], expert_weight_ref[1:2, :]
    first_even = choice_ref[0:1, :] == 0
    scale = group_weight_ref[...].reshape(1, -1)
    both = first + second
    even_row = scale * jnp.where(first_even, first, second) / both
    odd_row = scale * jnp.where(first_even, second, first) / both
    seat_int = column(seat_row).astype(jnp.int32)
    taken = seat_int == lane
    mix_rows[0:1, :] = jnp.sum(jnp.where(taken, column(even_row), 0.0), 0, keepdims=True)
    mix_rows[1:2, :] = jnp.sum(jnp.where(taken, column(odd_row), 0.0), 0, keepdims=True)
    mix_send.start()
    wide = lax.broadcasted_iota(jnp.int32, (count, size), 1)
    for c in range(2 * chunks):
        place[c] = jnp.where(seat_int == wide + c * size, 1.0, 0.0).astype(jnp.bfloat16)
    for i in range(items + 2):
        if i < items:
            stage_b(i)
        if i < 2 * chunks:
            stage_r(i + 2 * chunks)
        if i + 2 < items:
            stage_a(i + 2)
        if i == items - 1:
            for k in range(chunks - 1):
                spread(hid, k, h_send, h_recv, 0)
        if i - 2 >= chunks:
            stage_d(i - 2)
        if i < items:
            stage_c(i)
        if i == items - 1:
            spread(hid, chunks - 1, h_send, h_recv, 0)
        if i - 2 >= chunks:
            stage_e(i - 2)
        if i - 4 >= 2 * chunks:
            stage_j(i - 4)
    for k in range(chunks):
        stage_d(k)
    for n, k in enumerate(range(max(items - 2, 2 * chunks), items)):
        if n < chunks:
            stage_e(n)
        stage_j(k)
    for k in range(min(2, chunks), chunks):
        stage_e(k)
    result = jnp.zeros((count, width), jnp.float32)
    for c in range(chunks):
        done = joined(c, mix_rows[...], 0)
        result = result + jnp.dot(place[c], done, preferred_element_type=jnp.float32)
    for c in range(chunks):
        arrived(home.at[c], c_recv.at[c])
        done = home[c]
        result = result + jnp.dot(place[chunks + c], done, preferred_element_type=jnp.float32)
    out_ref[...] = result.astype(jnp.bfloat16)

    for c in range(chunks):
        own_send(c).wait_send()
        other_send(c).wait_send()
        back_send(chunks + c).wait_send()
    mix_send.wait_send()
    for k in range(items):
        spread(rows, k, x_send, x_recv, 3)
        spread(hid, k, h_send, h_recv, 3)

    @pl.when(is_inner)
    def _():
        for k in range(2 * chunks, items):
            relay(k).wait_send()
            comb_send(k).wait_send()

    @pl.when(is_outer)
    def _():
        for k in range(2 * chunks, items):
            back_send(k).wait_send()


CHUNKS = 2


def paired_body(
    tokens,
    group_choice,
    expert_choice,
    group_weight,
    expert_weight,
    norm_gain,
    w_gate,
    w_up,
    w_down,
):
    count, width = tokens.shape
    half = count // 2
    depth, hidden_width = w_gate.shape[1:]
    chunks = CHUNKS if half % (16 * CHUNKS) == 0 else 1
    size = half // chunks
    items = 4 * chunks
    bf16 = jnp.bfloat16
    dma = pltpu.SemaphoreType.DMA
    vmem = pl.BlockSpec(memory_space=pltpu.VMEM)
    hbm = pl.BlockSpec(memory_space=pltpu.HBM)
    return pl.pallas_call(
        functools.partial(layer_kernel, chunks),
        out_shape=jax.ShapeDtypeStruct((count, width), bf16),
        in_specs=[hbm] * 9,
        out_specs=vmem,
        scratch_shapes=[
            pltpu.VMEM((count,), jnp.int32),
            pltpu.VMEM((2, count), jnp.int32),
            pltpu.VMEM((count,), jnp.float32),
            pltpu.VMEM((2, count), jnp.float32),
            pltpu.VMEM((1, norm_gain.shape[0]), jnp.float32),
            pltpu.VMEM((count, width), bf16),
            pltpu.VMEM((depth, hidden_width), bf16),
            pltpu.VMEM((depth, hidden_width), bf16),
            pltpu.VMEM(w_down.shape[1:], bf16),
            pltpu.VMEM((items, 4, size, width), bf16),
            pltpu.VMEM((chunks, size, width), bf16),
            pltpu.VMEM((items, 4, size, hidden_width), bf16),
            pltpu.VMEM((items, size, width), bf16),
            pltpu.VMEM((items, size, width), bf16),
            pltpu.VMEM((chunks, size, width), bf16),
            pltpu.VMEM((2 * chunks, count, size), bf16),
            pltpu.VMEM((2 * chunks, size, width), bf16),
            pltpu.VMEM((8, count), jnp.float32),
            pltpu.VMEM((2, 8, count), jnp.float32),
            pltpu.VMEM((size, depth), bf16),
            dma((9,)),
            dma((2 * chunks,)),
            dma((items,)),
            dma((2 * chunks,)),
            dma((items, 3)),
            dma((items, 3)),
            dma((items, 3)),
            dma((items, 3)),
            dma((items,)),
            dma((items,)),
            dma((2 * chunks,)),
            dma((chunks,)),
            dma,
            dma((2,)),
        ],
        compiler_params=pltpu.CompilerParams(
            collective_id=0, has_side_effects=True, vmem_limit_bytes=24 * 1024 * 1024
        ),
    )(
        *[pltpu.with_memory_space_constraint(x, pltpu.HBM) for x in (
        group_choice,
        expert_choice.T,
        group_weight,
        expert_weight.T,
        norm_gain.reshape(1, -1),
        tokens,
        w_gate[0],
        w_up[0],
        w_down[0],
    )])

def pick_body(mesh, *arrays):
    experts = arrays[6].shape[0]
    group_size = min(8, experts // 2)
    choices = arrays[2].shape[1]
    sizes = dict(mesh.shape)
    fits = group_size == choices and experts == 2 * group_size == sizes["ep"]
    return paired_body if fits and sizes["tp"] == sizes["ep"] else body


def solution(mesh):
    in_specs = (
        P(("grp", "ep"), "tp"),
        P(("grp", "ep")),
        P(("grp", "ep"), None),
        P(("grp", "ep")),
        P(("grp", "ep"), None),
        P(),
        P("ep", None, "tp"),
        P("ep", None, "tp"),
        P("ep", None, "tp"),
    )
    out_specs = P(("grp", "ep"), "tp")

    def layer(*arrays):
        run = jax.shard_map(
            pick_body(mesh, *arrays),
            mesh=mesh,
            in_specs=in_specs,
            out_specs=out_specs,
            check_vma=False,
        )
        return run(*arrays)

    return layer
```

```python
import functools

import jax
import jax.numpy as jnp
from jax import lax
from jax.experimental import pallas as pl
from jax.experimental.pallas import tpu as pltpu
from jax.sharding import PartitionSpec as P

MESH = pl.DeviceIdType.MESH


def finish_rows(gate_sum, up_sum, w_down):
    hidden = (jax.nn.silu(gate_sum) * up_sum).astype(jnp.bfloat16)
    whole_hidden = lax.all_gather(hidden, "tp", axis=3, tiled=True)
    summed = jnp.einsum("sxcf,xfd->sxcd", whole_hidden, w_down, preferred_element_type=jnp.float32)
    return summed.astype(jnp.bfloat16)


def body(
    tokens,
    group_choice,
    expert_choice,
    group_weight,
    expert_weight,
    norm_gain,
    w_gate,
    w_up,
    w_down,
):
    tok_rows = tokens.shape[0]
    ep_count = lax.axis_size("ep")
    exp_local = w_gate.shape[0]
    experts_all = ep_count * exp_local
    group_size = min(8, experts_all // 2)
    group_count = experts_all // group_size
    mean_load = 2 * tok_rows // experts_all
    capacity = mean_load + min(mean_load // 2, tok_rows // group_count - mean_load)
    model_width = norm_gain.shape[0]
    expert_ids = group_choice[:, None] * group_size + expert_choice
    mixing = group_weight[:, None] * expert_weight / jnp.sum(expert_weight, -1, keepdims=True)
    flat_ids = expert_ids.reshape(-1)
    marks = (flat_ids[:, None] == jnp.arange(experts_all, dtype=jnp.int32)[None, :]).astype(
        jnp.int32
    )
    earlier = jnp.cumsum(marks, 0) - marks
    seat_index = jnp.sum(earlier * marks, 1)
    targets = (flat_ids * capacity + seat_index).reshape(tok_rows, 2)
    places = jnp.arange(experts_all * capacity, dtype=jnp.int32)
    dispatch = (
        (places[:, None] == targets[None, :, 0]) | (places[:, None] == targets[None, :, 1])
    ).astype(jnp.bfloat16)
    values = tokens.astype(jnp.float32)
    own_squares = jnp.sum(values * values, -1)
    all_squares = lax.psum(own_squares, "tp")
    inv_rms = lax.rsqrt(all_squares / model_width + 1e-06)
    piece_width = tokens.shape[1]
    gain_piece = lax.dynamic_slice_in_dim(
        norm_gain, lax.axis_index("tp") * piece_width, piece_width, 0
    )
    normed = (values * inv_rms[:, None] * gain_piece[None, :]).astype(jnp.bfloat16)
    buffer = jnp.dot(dispatch, normed, preferred_element_type=jnp.float32).astype(jnp.bfloat16)
    buffer = buffer.reshape(ep_count, exp_local, capacity, piece_width)
    piece = lax.all_gather(
        lax.all_to_all(buffer, "ep", split_axis=0, concat_axis=0, tiled=True),
        "tp",
        axis=3,
        tiled=True,
    )
    gate_next = jnp.einsum("sxcd,xdf->sxcf", piece, w_gate, preferred_element_type=jnp.float32)
    up_next = jnp.einsum("sxcd,xdf->sxcf", piece, w_up, preferred_element_type=jnp.float32)
    results = finish_rows(gate_next, up_next, w_down)
    returned = lax.all_to_all(results, "ep", split_axis=0, concat_axis=0, tiled=True)
    returned = returned.reshape(experts_all * capacity, returned.shape[3])
    combined = jnp.zeros((tok_rows, returned.shape[1]), jnp.float32)
    for choice_index in range(2):
        picker = (targets[:, choice_index : choice_index + 1] == places[None, :]).astype(
            jnp.bfloat16
        )
        picked = jnp.dot(picker, returned, preferred_element_type=jnp.float32)
        combined = combined + mixing[:, choice_index : choice_index + 1] * picked
    return combined.astype(jnp.bfloat16)


def layer_kernel(
    chunks,
    fine,
    group_hbm,
    choice_hbm,
    group_weight_hbm,
    expert_weight_hbm,
    gain_hbm,
    tok_hbm,
    gate_hbm,
    up_hbm,
    down_hbm,
    out_ref,
    group_ref,
    choice_ref,
    group_weight_ref,
    expert_weight_ref,
    gain_ref,
    tok_ref,
    seat_ref,
    w_gate,
    w_up,
    w_down,
    rows,
    other,
    hid,
    outs,
    back,
    home,
    place,
    comb,
    mix_rows,
    mix_far,
    norm,
    wsem,
    z_send,
    z_recv,
    x_send,
    x_far,
    x_near,
    h_send,
    h_far,
    h_near,
    r_send,
    r_recv,
    c_send,
    c_recv,
    m_send,
    m_recv,
):
    z = lax.axis_index("ep")
    t = lax.axis_index("tp")
    group = z // 2
    parity = z % 2
    inner = (parity + group) % 2
    partner = z + 1 - 2 * parity
    cross = 2 - group
    cross_outer = 3 * (1 - group)
    near = t + 1 - 2 * (t % 2)
    far = (t + 2) % 4
    diag = (near + 2) % 4
    size, width = rows.shape[2:]
    half = size * fine
    each = fine // chunks
    count = 2 * half
    items = 4 * fine
    model_width = 4 * width
    hidden_width = hid.shape[3]

    pairs = (
        (gate_hbm, w_gate),
        (up_hbm, w_up),
        (down_hbm, w_down),
        (tok_hbm, tok_ref),
        (group_hbm, group_ref),
        (choice_hbm, choice_ref),
        (group_weight_hbm, group_weight_ref),
        (expert_weight_hbm, expert_weight_ref),
        (gain_hbm, gain_ref),
    )
    loads = [
        pltpu.make_async_copy(source, target, wsem.at[i])
        for i, (source, target) in enumerate(pairs)
    ]

    barrier = pltpu.get_barrier_semaphore()

    def greet(**where):
        pl.semaphore_signal(barrier, inc=1, device_id=where, device_id_type=MESH)

    greet(tp=near)
    greet(tp=far)
    greet(ep=partner)

    @pl.when(inner == 1)
    def _():
        greet(ep=cross)
        greet(ep=cross_outer)

    for i in (4, 3, 5, 6, 7, 8, 0, 1, 2):
        loads[i].start()

    def remote(source, target, send, recv, **where):
        return pltpu.make_async_remote_copy(
            src_ref=source,
            dst_ref=target,
            send_sem=send,
            recv_sem=recv,
            device_id=where,
            device_id_type=MESH,
        )

    def arrived(ref, sem):
        remote(ref, ref, sem, sem, tp=near).wait_recv()

    loads[4].wait()
    line = lax.broadcasted_iota(jnp.int32, (count, count), 0)
    lane = lax.broadcasted_iota(jnp.int32, (count, count), 1)
    own_row = jnp.where(group_ref[...].reshape(1, -1) == group, 1.0, 0.0)
    own_rows = jnp.broadcast_to(own_row, (8, count)).astype(jnp.bfloat16)
    earlier = jnp.where(line < lane, 1.0, 0.0).astype(jnp.bfloat16)
    before = jnp.dot(own_rows, earlier, preferred_element_type=jnp.float32)[0:1, :]
    at = lax.broadcasted_iota(jnp.int32, (1, count), 1).astype(jnp.float32)
    seat_row = jnp.where(own_row > 0.5, before, half + at - before)
    seat_ref[...] = seat_row

    def sort_half(start, target):
        want = lax.broadcasted_iota(jnp.int32, (half, count), 0) + start
        seat_ints = seat_ref[...].astype(jnp.int32)
        order = jnp.where(seat_ints == want, 1.0, 0.0).astype(jnp.bfloat16)
        part = jnp.dot(order, tok_ref[...], preferred_element_type=jnp.float32)
        for c in range(fine):
            target(c, part[c * size : (c + 1) * size].astype(jnp.bfloat16))

    def keep_own(c, value):
        rows[c, t] = value

    def keep_other(c, value):
        other[c] = value

    loads[3].wait()
    sort_half(0, keep_own)
    pl.semaphore_wait(barrier, 4)

    def drained(ref, sem):
        remote(ref, ref, sem, sem, tp=near).wait_send()

    def spread(buffer, k, send, over, beside):
        mine = buffer.at[k, t]
        remote(mine, mine, send, over, tp=far).start()
        remote(mine, mine, send, beside, tp=near).start()

    def pass_on(buffer, k, send, over, beside):
        theirs = buffer.at[k, far]
        arrived(theirs, over)
        remote(theirs, theirs, send, beside, tp=near).start()

    def normed(k):
        for i in range(each):
            item = k * each + i
            squares = jnp.zeros((size, 1), jnp.float32)
            for j in range(4):
                values = rows[item, j].astype(jnp.float32)
                squares = squares + jnp.sum(values * values, 1, keepdims=True)
            inv_rms = lax.rsqrt(squares / model_width + 1e-06)
            for j in range(4):
                cols = slice(j * width, (j + 1) * width)
                values = rows[item, j].astype(jnp.float32)
                norm[i * size : (i + 1) * size, cols] = (
                    values * inv_rms * gain_ref[0:1, cols]
                ).astype(jnp.bfloat16)

    def up_stage(k):
        gate = jnp.dot(norm[...], w_gate[...], preferred_element_type=jnp.float32)
        up = jnp.dot(norm[...], w_up[...], preferred_element_type=jnp.float32)
        hid[k, t] = (gate / (1.0 + jnp.exp(-gate)) * up).astype(jnp.bfloat16)

    def down_stage(k):
        total = jnp.zeros((size * each, width), jnp.float32)
        for j in range(4):
            part = w_down[j * hidden_width : (j + 1) * hidden_width, :]
            total = total + jnp.dot(hid[k, j], part, preferred_element_type=jnp.float32)
        for i in range(each):
            outs[k * each + i] = total[i * size : (i + 1) * size].astype(jnp.bfloat16)

    def mix_tables():
        first, second = expert_weight_ref[0:1, :], expert_weight_ref[1:2, :]
        first_even = choice_ref[0:1, :] == 0
        scale = group_weight_ref[...].reshape(1, -1)
        both = first + second
        even_row = scale * jnp.where(first_even, first, second) / both
        odd_row = scale * jnp.where(first_even, second, first) / both
        down = lax.broadcasted_iota(jnp.int32, (count, count), 0)
        over = lax.broadcasted_iota(jnp.int32, (count, count), 1)
        eye = down == over

        def column(row):
            return jnp.sum(jnp.where(eye, row, 0.0), 1, keepdims=True)

        seat_int = column(seat_ref[...]).astype(jnp.int32)
        taken = seat_int == over
        mix_rows[0:1, :] = jnp.sum(jnp.where(taken, column(even_row), 0.0), 0, keepdims=True)
        mix_rows[1:2, :] = jnp.sum(jnp.where(taken, column(odd_row), 0.0), 0, keepdims=True)
        wide = lax.broadcasted_iota(jnp.int32, (count, size), 1)
        for c in range(2 * fine):
            place[c] = jnp.where(seat_int == wide + c * size, 1.0, 0.0).astype(jnp.bfloat16)

    def joined(k, mixes, start, odd_first):
        start = start + (k % fine) * size
        low = lax.broadcasted_iota(jnp.int32, (size, count), 0) + start
        pick = low == lax.broadcasted_iota(jnp.int32, (size, count), 1)
        even = jnp.sum(jnp.where(pick, mixes[0:1, :], 0.0), 1, keepdims=True)
        odd = jnp.sum(jnp.where(pick, mixes[1:2, :], 0.0), 1, keepdims=True)
        mine, theirs = (odd, even) if odd_first else (even, odd)
        summed = mine * outs[k].astype(jnp.float32) + theirs * back[k].astype(jnp.float32)
        return summed.astype(jnp.bfloat16)

    def run(role):
        its_group, its_parity = role // 2, role % 2
        is_inner = (its_parity + its_group) % 2 == 1
        its_partner = role + 1 - 2 * its_parity
        its_cross = 2 - its_group
        its_cross_outer = 3 * (1 - its_group)
        slot = 2 if is_inner else 3
        waited = set()
        sums = [jnp.zeros((count, width), jnp.float32)]

        def once(name, wait):
            if name not in waited:
                waited.add(name)
                wait()

        def landed(k):
            once(("z", k), lambda: arrived(rows.at[k, t], z_recv.at[k - fine]))

        def send_row(source, k, place_at):
            sem = z_recv.at[k - fine]
            remote(source, rows.at[k, t], z_send, sem, ep=place_at).start()

        def send_back(k):
            there = k - fine if k < 2 * fine else k
            sem = r_recv.at[k - fine]
            remote(outs.at[k], back.at[there], r_send, sem, ep=its_partner).start()

        def send_home(k):
            where = its_cross if k < 3 * fine else its_cross_outer
            sem = c_recv.at[k % fine]
            remote(comb.at[k - 2 * fine], home.at[k % fine], c_send, sem, ep=where).start()

        def returned(k):
            arrived(back.at[k], r_recv.at[k if k < fine else k - fine])

        def act(step, k):
            if step == OWN:
                send_row(rows.at[k, t], fine + k, its_partner)
            elif step == SORT:
                sort_half(half, keep_other)
            elif step == OTHER:
                send_row(other.at[k], slot * fine + k, its_cross)
            elif step == MIX:
                for i in (5, 6, 7):
                    loads[i].wait()
                mix_tables()
                far_mix = mix_far.at[slot - 2]
                remote(mix_rows, far_mix, m_send, m_recv.at[slot - 2], ep=its_cross).start()
            elif step == ROW:
                if k >= fine:
                    landed(k)
                spread(rows, k, x_send, x_far.at[k], x_near.at[k // each])
            elif step == ROW_PASS:
                pass_on(rows, k, x_send, x_far.at[k], x_near.at[k // each])
            elif step == RELAY:
                landed(k)
                send_row(rows.at[k, t], k, its_partner)
            elif step == UP:
                arrived(rows.at[pl.ds(k * each, each), pl.ds(0, 2)], x_near.at[k])
                for i in (8, 0, 1):
                    once(("load", i), loads[i].wait)
                normed(k)
                up_stage(k)
            elif step == HID:
                spread(hid, k, h_send, h_far.at[k], h_near.at[k])
            elif step == HID_PASS:
                pass_on(hid, k, h_send, h_far.at[k], h_near.at[k])
            elif step == DOWN:
                arrived(hid.at[k, pl.ds(0, 2)], h_near.at[k])
                once(("load", 2), loads[2].wait)
                down_stage(k)
                if chunks <= k < 2 * chunks or (k >= 2 * chunks and not is_inner):
                    for i in range(each):
                        send_back(k * each + i)
            elif step == JOIN:
                i = k // fine - 2
                once(("mix", i), lambda: arrived(mix_far.at[i], m_recv.at[i]))
                returned(k)
                comb[k - 2 * fine] = joined(k, mix_far[i], half, its_parity)
                send_home(k)
            elif step == OWN_DONE:
                returned(k)
                done = joined(k, mix_rows[...], 0, its_parity)
                sums[0] += jnp.dot(place[k], done, preferred_element_type=jnp.float32)
            elif step == HOME_DONE:
                arrived(home.at[k], c_recv.at[k])
                done = home[k]
                sums[0] += jnp.dot(place[fine + k], done, preferred_element_type=jnp.float32)

        for step, k in PROGRAMS[role]:
            act(step, k)
        out_ref[...] = sums[0].astype(jnp.bfloat16)

        drained(rows.at[:, pl.ds(0, 3)], x_send)
        drained(hid.at[:, pl.ds(0, 3)], h_send)
        drained(mix_rows, m_send)
        if is_inner:
            drained(rows.at[pl.ds(0, fine)], z_send)
            drained(outs.at[pl.ds(0, fine)], r_send)
            drained(comb, c_send)
        else:
            drained(rows.at[pl.ds(0, fine), pl.ds(0, 2)], z_send)
            drained(outs.at[pl.ds(0, 3 * fine)], r_send)

    for role in range(len(PROGRAMS)):
        pl.when(z == role)(functools.partial(run, role))


CHUNKS = 3
FINE = 3
(
    OWN,
    SORT,
    OTHER,
    MIX,
    ROW,
    ROW_PASS,
    RELAY,
    UP,
    HID,
    HID_PASS,
    DOWN,
    JOIN,
    OWN_DONE,
    HOME_DONE,
) = range(14)
PROGRAMS = (
    (
        (ROW, 2),
        (OWN, 2),
        (ROW, 1),
        (SORT, 0),
        (OWN, 0),
        (ROW, 0),
        (OTHER, 1),
        (OTHER, 2),
        (ROW, 4),
        (ROW, 3),
        (OTHER, 0),
        (ROW, 7),
        (OWN, 1),
        (ROW_PASS, 4),
        (ROW, 5),
        (MIX, 0),
        (ROW, 10),
        (ROW, 8),
        (ROW_PASS, 3),
        (ROW_PASS, 1),
        (ROW_PASS, 7),
        (UP, 7),
        (HID, 7),
        (ROW, 11),
        (ROW_PASS, 0),
        (UP, 4),
        (ROW_PASS, 5),
        (ROW_PASS, 10),
        (UP, 1),
        (ROW_PASS, 8),
        (ROW, 6),
        (ROW_PASS, 2),
        (HID_PASS, 7),
        (UP, 8),
        (HID, 8),
        (UP, 10),
        (ROW_PASS, 11),
        (HID, 10),
        (DOWN, 7),
        (ROW, 9),
        (UP, 2),
        (UP, 11),
        (HID, 11),
        (HID, 4),
        (ROW_PASS, 6),
        (HID_PASS, 8),
        (UP, 3),
        (HID, 1),
        (DOWN, 8),
        (HID_PASS, 10),
        (UP, 0),
        (UP, 6),
        (HID, 6),
        (DOWN, 10),
        (HID_PASS, 11),
        (ROW_PASS, 9),
        (HID, 0),
        (UP, 5),
        (HID, 3),
        (DOWN, 11),
        (HID_PASS, 4),
        (UP, 9),
        (HID, 9),
        (HID_PASS, 1),
        (HID_PASS, 6),
        (DOWN, 4),
        (HID, 2),
        (DOWN, 1),
        (HID_PASS, 0),
        (HID, 5),
        (DOWN, 6),
        (HID_PASS, 3),
        (HID_PASS, 9),
        (DOWN, 0),
        (DOWN, 9),
        (HOME_DONE, 1),
        (HID_PASS, 2),
        (HID_PASS, 5),
        (DOWN, 3),
        (HOME_DONE, 2),
        (DOWN, 2),
        (DOWN, 5),
        (OWN_DONE, 0),
        (HOME_DONE, 0),
        (OWN_DONE, 2),
        (OWN_DONE, 1),
    ),
    (
        (ROW, 2),
        (OWN, 1),
        (OWN, 0),
        (OWN, 2),
        (SORT, 0),
        (ROW, 1),
        (ROW, 0),
        (OTHER, 1),
        (OTHER, 2),
        (ROW, 5),
        (RELAY, 7),
        (RELAY, 10),
        (ROW, 10),
        (ROW, 3),
        (ROW_PASS, 5),
        (RELAY, 8),
        (ROW, 8),
        (ROW_PASS, 2),
        (UP, 5),
        (OTHER, 0),
        (ROW_PASS, 1),
        (HID, 5),
        (ROW, 11),
        (RELAY, 11),
        (ROW, 7),
        (ROW_PASS, 3),
        (RELAY, 6),
        (ROW, 6),
        (ROW_PASS, 8),
        (HID_PASS, 5),
        (ROW_PASS, 0),
        (UP, 3),
        (RELAY, 9),
        (DOWN, 5),
        (HID, 3),
        (UP, 2),
        (ROW_PASS, 10),
        (UP, 8),
        (ROW_PASS, 7),
        (ROW, 4),
        (UP, 1),
        (ROW, 9),
        (UP, 10),
        (ROW_PASS, 6),
        (UP, 7),
        (HID_PASS, 3),
        (HID, 7),
        (ROW_PASS, 11),
        (HID, 2),
        (HID, 8),
        (HID, 10),
        (UP, 0),
        (DOWN, 3),
        (MIX, 0),
        (ROW_PASS, 4),
        (UP, 6),
        (ROW_PASS, 9),
        (UP, 11),
        (HID, 1),
        (HID, 6),
        (HID, 11),
        (HID_PASS, 7),
        (UP, 4),
        (HID_PASS, 2),
        (HID, 0),
        (DOWN, 7),
        (JOIN, 7),
        (HID_PASS, 8),
        (HID, 4),
        (DOWN, 2),
        (HID_PASS, 10),
        (DOWN, 8),
        (JOIN, 8),
        (HID_PASS, 1),
        (DOWN, 10),
        (UP, 9),
        (HID, 9),
        (HID_PASS, 11),
        (JOIN, 10),
        (DOWN, 1),
        (HID_PASS, 4),
        (HID_PASS, 6),
        (HID_PASS, 0),
        (DOWN, 11),
        (JOIN, 11),
        (DOWN, 0),
        (DOWN, 6),
        (DOWN, 4),
        (HID_PASS, 9),
        (JOIN, 6),
        (DOWN, 9),
        (OWN_DONE, 1),
        (JOIN, 9),
        (HOME_DONE, 1),
        (HOME_DONE, 2),
        (OWN_DONE, 0),
        (OWN_DONE, 2),
        (HOME_DONE, 0),
    ),
    (
        (ROW, 2),
        (ROW, 1),
        (OWN, 2),
        (SORT, 0),
        (OWN, 0),
        (OTHER, 1),
        (RELAY, 7),
        (OTHER, 2),
        (ROW, 7),
        (OWN, 1),
        (ROW, 3),
        (ROW, 0),
        (ROW_PASS, 2),
        (ROW_PASS, 1),
        (RELAY, 10),
        (RELAY, 8),
        (OTHER, 0),
        (ROW, 10),
        (RELAY, 11),
        (ROW_PASS, 7),
        (ROW, 11),
        (UP, 7),
        (HID, 7),
        (ROW, 8),
        (RELAY, 9),
        (ROW, 4),
        (ROW_PASS, 0),
        (UP, 2),
        (HID_PASS, 7),
        (RELAY, 6),
        (ROW_PASS, 10),
        (ROW, 5),
        (ROW_PASS, 3),
        (ROW_PASS, 11),
        (DOWN, 7),
        (ROW, 9),
        (UP, 3),
        (UP, 11),
        (HID, 11),
        (ROW_PASS, 4),
        (ROW_PASS, 8),
        (UP, 0),
        (HID, 3),
        (MIX, 0),
        (ROW_PASS, 5),
        (UP, 10),
        (UP, 1),
        (HID, 10),
        (ROW_PASS, 9),
        (UP, 5),
        (HID, 5),
        (HID_PASS, 11),
        (ROW, 6),
        (HID, 0),
        (HID_PASS, 3),
        (UP, 9),
        (DOWN, 11),
        (HID, 9),
        (HID_PASS, 10),
        (DOWN, 3),
        (UP, 4),
        (HID, 1),
        (HID_PASS, 5),
        (DOWN, 10),
        (UP, 8),
        (DOWN, 5),
        (HID, 8),
        (HID, 4),
        (ROW_PASS, 6),
        (HID, 2),
        (JOIN, 10),
        (HID_PASS, 9),
        (HID_PASS, 0),
        (UP, 6),
        (HID, 6),
        (HID_PASS, 1),
        (JOIN, 11),
        (HOME_DONE, 1),
        (DOWN, 0),
        (HID_PASS, 8),
        (DOWN, 9),
        (DOWN, 1),
        (HID_PASS, 4),
        (JOIN, 9),
        (HOME_DONE, 2),
        (HID_PASS, 2),
        (DOWN, 8),
        (HID_PASS, 6),
        (JOIN, 7),
        (DOWN, 4),
        (DOWN, 2),
        (DOWN, 6),
        (JOIN, 8),
        (JOIN, 6),
        (HOME_DONE, 0),
        (OWN_DONE, 1),
        (OWN_DONE, 0),
        (OWN_DONE, 2),
    ),
    (
        (ROW, 1),
        (OWN, 0),
        (ROW, 2),
        (SORT, 0),
        (ROW, 0),
        (MIX, 0),
        (OTHER, 1),
        (ROW, 5),
        (OTHER, 2),
        (ROW, 3),
        (ROW_PASS, 1),
        (ROW, 7),
        (ROW_PASS, 0),
        (OWN, 1),
        (OTHER, 0),
        (ROW_PASS, 2),
        (UP, 1),
        (OWN, 2),
        (ROW, 10),
        (ROW, 8),
        (UP, 0),
        (ROW_PASS, 3),
        (ROW_PASS, 7),
        (ROW, 11),
        (ROW, 4),
        (ROW_PASS, 5),
        (UP, 5),
        (ROW, 9),
        (ROW_PASS, 10),
        (UP, 7),
        (ROW_PASS, 8),
        (UP, 10),
        (HID, 10),
        (ROW_PASS, 11),
        (ROW_PASS, 4),
        (ROW, 6),
        (UP, 8),
        (UP, 3),
        (ROW_PASS, 9),
        (UP, 11),
        (HID, 11),
        (UP, 9),
        (HID, 9),
        (HID_PASS, 10),
        (HID, 7),
        (HID, 8),
        (DOWN, 10),
        (ROW_PASS, 6),
        (HID, 0),
        (HID, 1),
        (HID, 5),
        (HID_PASS, 11),
        (UP, 4),
        (HID_PASS, 9),
        (DOWN, 11),
        (HID_PASS, 7),
        (UP, 6),
        (HID_PASS, 8),
        (HID, 4),
        (DOWN, 9),
        (UP, 2),
        (HID_PASS, 0),
        (HID, 6),
        (DOWN, 7),
        (DOWN, 8),
        (HID_PASS, 1),
        (HID, 3),
        (DOWN, 0),
        (HID, 2),
        (HID_PASS, 5),
        (DOWN, 1),
        (HID_PASS, 6),
        (HID_PASS, 4),
        (DOWN, 6),
        (HID_PASS, 3),
        (DOWN, 4),
        (HID_PASS, 2),
        (HOME_DONE, 1),
        (DOWN, 3),
        (DOWN, 5),
        (DOWN, 2),
        (HOME_DONE, 2),
        (OWN_DONE, 2),
        (OWN_DONE, 1),
        (OWN_DONE, 0),
        (HOME_DONE, 0),
    ),
)


def paired_body(
    tokens,
    group_choice,
    expert_choice,
    group_weight,
    expert_weight,
    norm_gain,
    w_gate,
    w_up,
    w_down,
):
    count, width = tokens.shape
    half = count // 2
    depth, hidden_width = w_gate.shape[1:]
    chunks, fine = CHUNKS, FINE
    size = half // fine
    items = 4 * fine
    bf16 = jnp.bfloat16
    dma = pltpu.SemaphoreType.DMA
    vmem = pl.BlockSpec(memory_space=pltpu.VMEM)
    hbm = pl.BlockSpec(memory_space=pltpu.HBM)
    return pl.pallas_call(
        functools.partial(layer_kernel, chunks, fine),
        out_shape=jax.ShapeDtypeStruct((count, width), bf16),
        in_specs=[hbm] * 9,
        out_specs=vmem,
        scratch_shapes=[
            pltpu.VMEM((count,), jnp.int32),
            pltpu.VMEM((2, count), jnp.int32),
            pltpu.VMEM((count,), jnp.float32),
            pltpu.VMEM((2, count), jnp.float32),
            pltpu.VMEM((1, norm_gain.shape[0]), jnp.float32),
            pltpu.VMEM((count, width), bf16),
            pltpu.VMEM((1, count), jnp.float32),
            pltpu.VMEM((depth, hidden_width), bf16),
            pltpu.VMEM((depth, hidden_width), bf16),
            pltpu.VMEM(w_down.shape[1:], bf16),
            pltpu.VMEM((items, 4, size, width), bf16),
            pltpu.VMEM((fine, size, width), bf16),
            pltpu.VMEM((4 * chunks, 4, half // chunks, hidden_width), bf16),
            pltpu.VMEM((items, size, width), bf16),
            pltpu.VMEM((items, size, width), bf16),
            pltpu.VMEM((fine, size, width), bf16),
            pltpu.VMEM((2 * fine, count, size), bf16),
            pltpu.VMEM((2 * fine, size, width), bf16),
            pltpu.VMEM((8, count), jnp.float32),
            pltpu.VMEM((2, 8, count), jnp.float32),
            pltpu.VMEM((half // chunks, depth), bf16),
            dma((9,)),
            dma,
            dma((3 * fine,)),
            dma,
            dma((items,)),
            dma((4 * chunks,)),
            dma,
            dma((4 * chunks,)),
            dma((4 * chunks,)),
            dma,
            dma((3 * fine,)),
            dma,
            dma((fine,)),
            dma,
            dma((2,)),
        ],
        compiler_params=pltpu.CompilerParams(
            collective_id=0, has_side_effects=True, vmem_limit_bytes=24 * 1024 * 1024
        ),
    )(
        *[pltpu.with_memory_space_constraint(x, pltpu.HBM) for x in (
        group_choice,
        expert_choice.T,
        group_weight,
        expert_weight.T,
        norm_gain.reshape(1, -1),
        tokens,
        w_gate[0],
        w_up[0],
        w_down[0],
    )])


def pick_body(mesh, *arrays):
    experts = arrays[6].shape[0]
    group_size = min(8, experts // 2)
    choices = arrays[2].shape[1]
    sizes = dict(mesh.shape)
    fits = group_size == choices and experts == 2 * group_size == sizes["ep"]
    fits = fits and sizes["tp"] == sizes["ep"] == len(PROGRAMS)
    fits = fits and arrays[0].shape[0] % (32 * FINE) == 0
    return paired_body if fits else body


def solution(mesh):
    in_specs = (
        P(("grp", "ep"), "tp"),
        P(("grp", "ep")),
        P(("grp", "ep"), None),
        P(("grp", "ep")),
        P(("grp", "ep"), None),
        P(),
        P("ep", None, "tp"),
        P("ep", None, "tp"),
        P("ep", None, "tp"),
    )
    out_specs = P(("grp", "ep"), "tp")

    def layer(*arrays):
        run = jax.shard_map(
            pick_body(mesh, *arrays),
            mesh=mesh,
            in_specs=in_specs,
            out_specs=out_specs,
            check_vma=False,
        )
        return run(*arrays)

    return layer
```

```python
import functools

import jax
import jax.numpy as jnp
from jax import lax
from jax.experimental import pallas as pl
from jax.experimental.pallas import tpu as pltpu
from jax.sharding import PartitionSpec as P

MESH = pl.DeviceIdType.MESH


def finish_rows(gate_sum, up_sum, w_down):
    hidden = (jax.nn.silu(gate_sum) * up_sum).astype(jnp.bfloat16)
    whole_hidden = lax.all_gather(hidden, "tp", axis=3, tiled=True)
    summed = jnp.einsum("sxcf,xfd->sxcd", whole_hidden, w_down, preferred_element_type=jnp.float32)
    return summed.astype(jnp.bfloat16)


def body(
    tokens,
    group_choice,
    expert_choice,
    group_weight,
    expert_weight,
    norm_gain,
    w_gate,
    w_up,
    w_down,
):
    tok_rows = tokens.shape[0]
    ep_count = lax.axis_size("ep")
    exp_local = w_gate.shape[0]
    experts_all = ep_count * exp_local
    group_size = min(8, experts_all // 2)
    group_count = experts_all // group_size
    mean_load = 2 * tok_rows // experts_all
    capacity = mean_load + min(mean_load // 2, tok_rows // group_count - mean_load)
    model_width = norm_gain.shape[0]
    expert_ids = group_choice[:, None] * group_size + expert_choice
    mixing = group_weight[:, None] * expert_weight / jnp.sum(expert_weight, -1, keepdims=True)
    flat_ids = expert_ids.reshape(-1)
    marks = (flat_ids[:, None] == jnp.arange(experts_all, dtype=jnp.int32)[None, :]).astype(
        jnp.int32
    )
    earlier = jnp.cumsum(marks, 0) - marks
    seat_index = jnp.sum(earlier * marks, 1)
    targets = (flat_ids * capacity + seat_index).reshape(tok_rows, 2)
    places = jnp.arange(experts_all * capacity, dtype=jnp.int32)
    dispatch = (
        (places[:, None] == targets[None, :, 0]) | (places[:, None] == targets[None, :, 1])
    ).astype(jnp.bfloat16)
    values = tokens.astype(jnp.float32)
    own_squares = jnp.sum(values * values, -1)
    all_squares = lax.psum(own_squares, "tp")
    inv_rms = lax.rsqrt(all_squares / model_width + 1e-06)
    piece_width = tokens.shape[1]
    gain_piece = lax.dynamic_slice_in_dim(
        norm_gain, lax.axis_index("tp") * piece_width, piece_width, 0
    )
    normed = (values * inv_rms[:, None] * gain_piece[None, :]).astype(jnp.bfloat16)
    buffer = jnp.dot(dispatch, normed, preferred_element_type=jnp.float32).astype(jnp.bfloat16)
    buffer = buffer.reshape(ep_count, exp_local, capacity, piece_width)
    piece = lax.all_gather(
        lax.all_to_all(buffer, "ep", split_axis=0, concat_axis=0, tiled=True),
        "tp",
        axis=3,
        tiled=True,
    )
    gate_next = jnp.einsum("sxcd,xdf->sxcf", piece, w_gate, preferred_element_type=jnp.float32)
    up_next = jnp.einsum("sxcd,xdf->sxcf", piece, w_up, preferred_element_type=jnp.float32)
    results = finish_rows(gate_next, up_next, w_down)
    returned = lax.all_to_all(results, "ep", split_axis=0, concat_axis=0, tiled=True)
    returned = returned.reshape(experts_all * capacity, returned.shape[3])
    combined = jnp.zeros((tok_rows, returned.shape[1]), jnp.float32)
    for choice_index in range(2):
        picker = (targets[:, choice_index : choice_index + 1] == places[None, :]).astype(
            jnp.bfloat16
        )
        picked = jnp.dot(picker, returned, preferred_element_type=jnp.float32)
        combined = combined + mixing[:, choice_index : choice_index + 1] * picked
    return combined.astype(jnp.bfloat16)


def layer_kernel(
    chunks,
    fine,
    group_hbm,
    choice_hbm,
    group_weight_hbm,
    expert_weight_hbm,
    gain_hbm,
    tok_hbm,
    gate_hbm,
    up_hbm,
    down_hbm,
    out_ref,
    group_ref,
    choice_ref,
    group_weight_ref,
    expert_weight_ref,
    gain_ref,
    tok_ref,
    seat_ref,
    w_gate,
    w_up,
    w_down,
    rows,
    other,
    hid,
    outs,
    back,
    home,
    place,
    comb,
    mix_rows,
    mix_far,
    norm,
    wsem,
    z_send,
    z_recv,
    x_send,
    x_far,
    x_near,
    h_send,
    h_far,
    h_near,
    r_send,
    r_recv,
    c_send,
    c_recv,
    m_send,
    m_recv,
):
    z = lax.axis_index("ep")
    t = lax.axis_index("tp")
    group = z // 2
    parity = z % 2
    inner = (parity + group) % 2
    partner = z + 1 - 2 * parity
    cross = 2 - group
    cross_outer = 3 * (1 - group)
    near = t + 1 - 2 * (t % 2)
    far = (t + 2) % 4
    diag = (near + 2) % 4
    size, width = rows.shape[2:]
    half = size * fine
    each = fine // chunks
    count = 2 * half
    items = 4 * fine
    model_width = 4 * width
    hidden_width = hid.shape[3]

    pairs = (
        (gate_hbm, w_gate),
        (up_hbm, w_up),
        (down_hbm, w_down),
        (tok_hbm, tok_ref),
        (group_hbm, group_ref),
        (choice_hbm, choice_ref),
        (group_weight_hbm, group_weight_ref),
        (expert_weight_hbm, expert_weight_ref),
        (gain_hbm, gain_ref),
    )
    loads = [
        pltpu.make_async_copy(source, target, wsem.at[i])
        for i, (source, target) in enumerate(pairs)
    ]

    barrier = pltpu.get_barrier_semaphore()

    def greet(**where):
        pl.semaphore_signal(barrier, inc=1, device_id=where, device_id_type=MESH)

    greet(tp=near)
    greet(tp=far)
    greet(ep=partner)

    @pl.when(inner == 1)
    def _():
        greet(ep=cross)
        greet(ep=cross_outer)

    for i in (4, 3, 5, 6, 7, 8, 0, 1, 2):
        loads[i].start()

    def remote(source, target, send, recv, **where):
        return pltpu.make_async_remote_copy(
            src_ref=source,
            dst_ref=target,
            send_sem=send,
            recv_sem=recv,
            device_id=where,
            device_id_type=MESH,
        )

    def arrived(ref, sem):
        remote(ref, ref, sem, sem, tp=near).wait_recv()

    loads[4].wait()
    line = lax.broadcasted_iota(jnp.int32, (count, count), 0)
    lane = lax.broadcasted_iota(jnp.int32, (count, count), 1)
    own_row = jnp.where(group_ref[...].reshape(1, -1) == group, 1.0, 0.0)
    own_rows = jnp.broadcast_to(own_row, (8, count)).astype(jnp.bfloat16)
    earlier = jnp.where(line < lane, 1.0, 0.0).astype(jnp.bfloat16)
    before = jnp.dot(own_rows, earlier, preferred_element_type=jnp.float32)[0:1, :]
    at = lax.broadcasted_iota(jnp.int32, (1, count), 1).astype(jnp.float32)
    seat_row = jnp.where(own_row > 0.5, before, half + at - before)
    seat_ref[...] = seat_row

    def sort_half(start, target):
        want = lax.broadcasted_iota(jnp.int32, (half, count), 0) + start
        seat_ints = seat_ref[...].astype(jnp.int32)
        order = jnp.where(seat_ints == want, 1.0, 0.0).astype(jnp.bfloat16)
        part = jnp.dot(order, tok_ref[...], preferred_element_type=jnp.float32)
        for c in range(fine):
            target(c, part[c * size : (c + 1) * size].astype(jnp.bfloat16))

    def keep_own(c, value):
        rows[c, t] = value

    def keep_other(c, value):
        other[c] = value

    loads[3].wait()
    sort_half(0, keep_own)
    pl.semaphore_wait(barrier, 4)

    def drained(ref, sem):
        remote(ref, ref, sem, sem, tp=near).wait_send()

    def spread(buffer, k, send, over, beside):
        mine = buffer.at[k, t]
        remote(mine, mine, send, over, tp=far).start()
        remote(mine, mine, send, beside, tp=near).start()

    def pass_on(buffer, k, send, over, beside):
        theirs = buffer.at[k, far]
        arrived(theirs, over)
        remote(theirs, theirs, send, beside, tp=near).start()

    def normed(k):
        for i in range(each):
            item = k * each + i
            squares = jnp.zeros((size, 1), jnp.float32)
            for j in range(4):
                values = rows[item, j].astype(jnp.float32)
                squares = squares + jnp.sum(values * values, 1, keepdims=True)
            inv_rms = lax.rsqrt(squares / model_width + 1e-06)
            for j in range(4):
                cols = slice(j * width, (j + 1) * width)
                values = rows[item, j].astype(jnp.float32)
                norm[i * size : (i + 1) * size, cols] = (
                    values * inv_rms * gain_ref[0:1, cols]
                ).astype(jnp.bfloat16)

    def up_stage(k):
        gate = jnp.dot(norm[...], w_gate[...], preferred_element_type=jnp.float32)
        up = jnp.dot(norm[...], w_up[...], preferred_element_type=jnp.float32)
        hid[k, t] = (gate / (1.0 + jnp.exp(-gate)) * up).astype(jnp.bfloat16)

    def down_stage(k):
        total = jnp.zeros((size * each, width), jnp.float32)
        for j in range(4):
            part = w_down[j * hidden_width : (j + 1) * hidden_width, :]
            total = total + jnp.dot(hid[k, j], part, preferred_element_type=jnp.float32)
        for i in range(each):
            outs[k * each + i] = total[i * size : (i + 1) * size].astype(jnp.bfloat16)

    def mix_tables():
        first, second = expert_weight_ref[0:1, :], expert_weight_ref[1:2, :]
        first_even = choice_ref[0:1, :] == 0
        scale = group_weight_ref[...].reshape(1, -1)
        both = first + second
        even_row = scale * jnp.where(first_even, first, second) / both
        odd_row = scale * jnp.where(first_even, second, first) / both
        down = lax.broadcasted_iota(jnp.int32, (count, count), 0)
        over = lax.broadcasted_iota(jnp.int32, (count, count), 1)
        eye = down == over

        def column(row):
            return jnp.sum(jnp.where(eye, row, 0.0), 1, keepdims=True)

        seat_int = column(seat_ref[...]).astype(jnp.int32)
        taken = seat_int == over
        mix_rows[0:1, :] = jnp.sum(jnp.where(taken, column(even_row), 0.0), 0, keepdims=True)
        mix_rows[1:2, :] = jnp.sum(jnp.where(taken, column(odd_row), 0.0), 0, keepdims=True)
        wide = lax.broadcasted_iota(jnp.int32, (count, size), 1)
        for c in range(2 * fine):
            place[c] = jnp.where(seat_int == wide + c * size, 1.0, 0.0).astype(jnp.bfloat16)

    def joined(k, mixes, start, odd_first):
        start = start + (k % fine) * size
        low = lax.broadcasted_iota(jnp.int32, (size, count), 0) + start
        pick = low == lax.broadcasted_iota(jnp.int32, (size, count), 1)
        even = jnp.sum(jnp.where(pick, mixes[0:1, :], 0.0), 1, keepdims=True)
        odd = jnp.sum(jnp.where(pick, mixes[1:2, :], 0.0), 1, keepdims=True)
        mine, theirs = (odd, even) if odd_first else (even, odd)
        summed = mine * outs[k].astype(jnp.float32) + theirs * back[k].astype(jnp.float32)
        return summed.astype(jnp.bfloat16)

    def run(role):
        its_group, its_parity = role // 2, role % 2
        is_inner = (its_parity + its_group) % 2 == 1
        its_partner = role + 1 - 2 * its_parity
        its_cross = 2 - its_group
        its_cross_outer = 3 * (1 - its_group)
        slot = 2 if is_inner else 3
        waited = set()
        sums = [jnp.zeros((count, width), jnp.float32)]

        def once(name, wait):
            if name not in waited:
                waited.add(name)
                wait()

        def landed(k):
            once(("z", k), lambda: arrived(rows.at[k, t], z_recv.at[k - fine]))

        def send_row(source, k, place_at):
            sem = z_recv.at[k - fine]
            remote(source, rows.at[k, t], z_send, sem, ep=place_at).start()

        def send_back(k):
            there = k - fine if k < 2 * fine else k
            sem = r_recv.at[k - fine]
            remote(outs.at[k], back.at[there], r_send, sem, ep=its_partner).start()

        def send_home(k):
            where = its_cross if k < 3 * fine else its_cross_outer
            sem = c_recv.at[k % fine]
            remote(comb.at[k - 2 * fine], home.at[k % fine], c_send, sem, ep=where).start()

        def returned(k):
            arrived(back.at[k], r_recv.at[k if k < fine else k - fine])

        def act(step, k):
            if step == OWN:
                send_row(rows.at[k, t], fine + k, its_partner)
            elif step == SORT:
                sort_half(half, keep_other)
            elif step == OTHER:
                send_row(other.at[k], slot * fine + k, its_cross)
            elif step == MIX:
                for i in (5, 6, 7):
                    loads[i].wait()
                mix_tables()
                far_mix = mix_far.at[slot - 2]
                remote(mix_rows, far_mix, m_send, m_recv.at[slot - 2], ep=its_cross).start()
            elif step == ROW:
                if k >= fine:
                    landed(k)
                spread(rows, k, x_send, x_far.at[k], x_near.at[k // each])
            elif step == ROW_PASS:
                pass_on(rows, k, x_send, x_far.at[k], x_near.at[k // each])
            elif step == RELAY:
                landed(k)
                send_row(rows.at[k, t], k, its_partner)
            elif step == UP:
                arrived(rows.at[pl.ds(k * each, each), pl.ds(0, 2)], x_near.at[k])
                for i in (8, 0, 1):
                    once(("load", i), loads[i].wait)
                normed(k)
                up_stage(k)
            elif step == HID:
                spread(hid, k, h_send, h_far.at[k], h_near.at[k])
            elif step == HID_PASS:
                pass_on(hid, k, h_send, h_far.at[k], h_near.at[k])
            elif step == DOWN:
                arrived(hid.at[k, pl.ds(0, 2)], h_near.at[k])
                once(("load", 2), loads[2].wait)
                down_stage(k)
                if chunks <= k < 2 * chunks or (k >= 2 * chunks and not is_inner):
                    for i in range(each):
                        send_back(k * each + i)
            elif step == JOIN:
                i = k // fine - 2
                once(("mix", i), lambda: arrived(mix_far.at[i], m_recv.at[i]))
                returned(k)
                comb[k - 2 * fine] = joined(k, mix_far[i], half, its_parity)
                send_home(k)
            elif step == OWN_DONE:
                returned(k)
                done = joined(k, mix_rows[...], 0, its_parity)
                sums[0] += jnp.dot(place[k], done, preferred_element_type=jnp.float32)
            elif step == HOME_DONE:
                arrived(home.at[k], c_recv.at[k])
                done = home[k]
                sums[0] += jnp.dot(place[fine + k], done, preferred_element_type=jnp.float32)

        for step, k in PROGRAMS[role]:
            act(step, k)
        out_ref[...] = sums[0].astype(jnp.bfloat16)

        drained(rows.at[:, pl.ds(0, 3)], x_send)
        drained(hid.at[:, pl.ds(0, 3)], h_send)
        drained(mix_rows, m_send)
        if is_inner:
            drained(rows.at[pl.ds(0, fine)], z_send)
            drained(outs.at[pl.ds(0, fine)], r_send)
            drained(comb, c_send)
        else:
            drained(rows.at[pl.ds(0, fine), pl.ds(0, 2)], z_send)
            drained(outs.at[pl.ds(0, 3 * fine)], r_send)

    for role in range(len(PROGRAMS)):
        pl.when(z == role)(functools.partial(run, role))


CHUNKS = 3
FINE = 3
(
    OWN,
    SORT,
    OTHER,
    MIX,
    ROW,
    ROW_PASS,
    RELAY,
    UP,
    HID,
    HID_PASS,
    DOWN,
    JOIN,
    OWN_DONE,
    HOME_DONE,
) = range(14)
PROGRAMS = (
    (
        (ROW, 2),
        (OWN, 2),
        (ROW, 1),
        (SORT, 0),
        (OWN, 0),
        (ROW, 0),
        (OTHER, 1),
        (OTHER, 2),
        (ROW, 4),
        (ROW, 3),
        (OTHER, 0),
        (ROW, 7),
        (OWN, 1),
        (ROW_PASS, 4),
        (ROW, 5),
        (MIX, 0),
        (ROW, 10),
        (ROW, 8),
        (ROW_PASS, 3),
        (ROW_PASS, 1),
        (ROW_PASS, 7),
        (UP, 7),
        (HID, 7),
        (ROW, 11),
        (ROW_PASS, 0),
        (UP, 4),
        (ROW_PASS, 5),
        (ROW_PASS, 10),
        (UP, 1),
        (ROW_PASS, 8),
        (ROW, 6),
        (ROW_PASS, 2),
        (HID_PASS, 7),
        (UP, 8),
        (HID, 8),
        (UP, 10),
        (ROW_PASS, 11),
        (HID, 10),
        (DOWN, 7),
        (ROW, 9),
        (UP, 2),
        (UP, 11),
        (HID, 11),
        (HID, 4),
        (ROW_PASS, 6),
        (HID_PASS, 8),
        (UP, 3),
        (HID, 1),
        (DOWN, 8),
        (HID_PASS, 10),
        (UP, 0),
        (UP, 6),
        (HID, 6),
        (DOWN, 10),
        (HID_PASS, 11),
        (ROW_PASS, 9),
        (HID, 0),
        (UP, 5),
        (HID, 3),
        (DOWN, 11),
        (HID_PASS, 4),
        (UP, 9),
        (HID, 9),
        (HID_PASS, 1),
        (HID_PASS, 6),
        (DOWN, 4),
        (HID, 5),
        (DOWN, 1),
        (HID_PASS, 0),
        (HID, 2),
        (DOWN, 6),
        (HID_PASS, 3),
        (HID_PASS, 9),
        (DOWN, 0),
        (DOWN, 9),
        (HOME_DONE, 1),
        (HID_PASS, 5),
        (HID_PASS, 2),
        (DOWN, 3),
        (DOWN, 5),
        (HOME_DONE, 2),
        (DOWN, 2),
        (OWN_DONE, 0),
        (HOME_DONE, 0),
        (OWN_DONE, 2),
        (OWN_DONE, 1),
    ),
    (
        (ROW, 2),
        (OWN, 1),
        (OWN, 0),
        (OWN, 2),
        (SORT, 0),
        (ROW, 1),
        (ROW, 0),
        (OTHER, 1),
        (OTHER, 2),
        (ROW, 5),
        (RELAY, 7),
        (RELAY, 10),
        (ROW, 10),
        (ROW, 3),
        (ROW_PASS, 5),
        (RELAY, 8),
        (ROW, 8),
        (ROW_PASS, 2),
        (UP, 5),
        (OTHER, 0),
        (ROW_PASS, 1),
        (HID, 5),
        (ROW, 11),
        (RELAY, 11),
        (ROW, 7),
        (ROW_PASS, 3),
        (RELAY, 6),
        (ROW, 6),
        (ROW_PASS, 8),
        (HID_PASS, 5),
        (ROW_PASS, 0),
        (UP, 3),
        (RELAY, 9),
        (DOWN, 5),
        (HID, 3),
        (UP, 2),
        (ROW_PASS, 10),
        (UP, 8),
        (ROW_PASS, 7),
        (ROW, 4),
        (UP, 1),
        (ROW, 9),
        (UP, 10),
        (ROW_PASS, 6),
        (UP, 7),
        (HID_PASS, 3),
        (HID, 7),
        (ROW_PASS, 11),
        (HID, 2),
        (HID, 8),
        (HID, 10),
        (UP, 0),
        (DOWN, 3),
        (MIX, 0),
        (ROW_PASS, 4),
        (UP, 6),
        (ROW_PASS, 9),
        (UP, 11),
        (HID, 1),
        (HID, 6),
        (HID, 11),
        (HID_PASS, 7),
        (UP, 4),
        (HID_PASS, 2),
        (HID, 0),
        (DOWN, 7),
        (JOIN, 7),
        (HID_PASS, 8),
        (HID, 4),
        (DOWN, 2),
        (HID_PASS, 10),
        (DOWN, 8),
        (JOIN, 8),
        (HID_PASS, 1),
        (DOWN, 10),
        (UP, 9),
        (HID, 9),
        (HID_PASS, 11),
        (JOIN, 10),
        (DOWN, 1),
        (HID_PASS, 4),
        (HID_PASS, 6),
        (HID_PASS, 0),
        (DOWN, 11),
        (DOWN, 4),
        (JOIN, 11),
        (DOWN, 0),
        (DOWN, 6),
        (HID_PASS, 9),
        (JOIN, 6),
        (DOWN, 9),
        (OWN_DONE, 1),
        (JOIN, 9),
        (HOME_DONE, 1),
        (HOME_DONE, 2),
        (OWN_DONE, 0),
        (OWN_DONE, 2),
        (HOME_DONE, 0),
    ),
    (
        (ROW, 2),
        (ROW, 1),
        (OWN, 2),
        (SORT, 0),
        (OWN, 0),
        (OTHER, 1),
        (RELAY, 7),
        (OTHER, 2),
        (ROW, 7),
        (OWN, 1),
        (ROW, 3),
        (ROW, 0),
        (ROW_PASS, 2),
        (ROW_PASS, 1),
        (RELAY, 10),
        (RELAY, 8),
        (OTHER, 0),
        (ROW, 10),
        (RELAY, 11),
        (ROW_PASS, 7),
        (ROW, 11),
        (UP, 7),
        (HID, 7),
        (ROW, 8),
        (RELAY, 9),
        (ROW, 4),
        (ROW_PASS, 0),
        (UP, 2),
        (HID_PASS, 7),
        (RELAY, 6),
        (ROW_PASS, 10),
        (ROW, 5),
        (ROW_PASS, 3),
        (ROW_PASS, 11),
        (DOWN, 7),
        (ROW, 9),
        (UP, 3),
        (UP, 11),
        (HID, 11),
        (ROW_PASS, 4),
        (ROW_PASS, 8),
        (UP, 0),
        (HID, 3),
        (MIX, 0),
        (ROW_PASS, 5),
        (UP, 10),
        (UP, 1),
        (HID, 10),
        (ROW_PASS, 9),
        (UP, 5),
        (HID, 5),
        (HID_PASS, 11),
        (ROW, 6),
        (HID, 0),
        (HID_PASS, 3),
        (UP, 9),
        (DOWN, 11),
        (HID, 9),
        (HID_PASS, 10),
        (DOWN, 3),
        (UP, 4),
        (HID, 1),
        (HID_PASS, 5),
        (DOWN, 10),
        (UP, 8),
        (DOWN, 5),
        (HID, 8),
        (HID, 4),
        (ROW_PASS, 6),
        (HID, 2),
        (JOIN, 10),
        (HID_PASS, 9),
        (HID_PASS, 0),
        (UP, 6),
        (HID, 6),
        (HID_PASS, 1),
        (JOIN, 11),
        (HOME_DONE, 1),
        (DOWN, 0),
        (HID_PASS, 8),
        (DOWN, 9),
        (DOWN, 1),
        (HID_PASS, 4),
        (JOIN, 9),
        (HOME_DONE, 2),
        (HID_PASS, 2),
        (DOWN, 8),
        (HID_PASS, 6),
        (JOIN, 7),
        (DOWN, 4),
        (DOWN, 2),
        (DOWN, 6),
        (JOIN, 8),
        (JOIN, 6),
        (HOME_DONE, 0),
        (OWN_DONE, 1),
        (OWN_DONE, 0),
        (OWN_DONE, 2),
    ),
    (
        (ROW, 1),
        (OWN, 0),
        (ROW, 2),
        (SORT, 0),
        (ROW, 0),
        (MIX, 0),
        (OTHER, 1),
        (ROW, 5),
        (OTHER, 2),
        (ROW, 3),
        (ROW_PASS, 1),
        (ROW, 7),
        (ROW_PASS, 0),
        (OWN, 1),
        (OTHER, 0),
        (ROW_PASS, 2),
        (UP, 1),
        (OWN, 2),
        (ROW, 10),
        (ROW, 8),
        (UP, 0),
        (ROW_PASS, 3),
        (ROW_PASS, 7),
        (ROW, 11),
        (ROW, 4),
        (ROW_PASS, 5),
        (UP, 5),
        (ROW, 9),
        (ROW_PASS, 10),
        (UP, 7),
        (ROW_PASS, 8),
        (UP, 10),
        (HID, 10),
        (ROW_PASS, 11),
        (ROW_PASS, 4),
        (ROW, 6),
        (UP, 8),
        (UP, 3),
        (ROW_PASS, 9),
        (UP, 11),
        (HID, 11),
        (UP, 9),
        (HID, 9),
        (HID_PASS, 10),
        (HID, 7),
        (HID, 8),
        (DOWN, 10),
        (ROW_PASS, 6),
        (HID, 0),
        (HID, 1),
        (HID, 5),
        (HID_PASS, 11),
        (UP, 4),
        (HID_PASS, 9),
        (DOWN, 11),
        (HID_PASS, 7),
        (UP, 6),
        (HID, 6),
        (HID_PASS, 8),
        (HID, 4),
        (DOWN, 9),
        (UP, 2),
        (HID_PASS, 0),
        (DOWN, 7),
        (DOWN, 8),
        (HID_PASS, 1),
        (HID, 3),
        (DOWN, 0),
        (HID, 2),
        (HID_PASS, 5),
        (DOWN, 1),
        (HID_PASS, 6),
        (HID_PASS, 4),
        (DOWN, 6),
        (HID_PASS, 3),
        (DOWN, 4),
        (HID_PASS, 2),
        (HOME_DONE, 1),
        (DOWN, 3),
        (DOWN, 5),
        (DOWN, 2),
        (HOME_DONE, 2),
        (OWN_DONE, 2),
        (OWN_DONE, 1),
        (OWN_DONE, 0),
        (HOME_DONE, 0),
    ),
)


def paired_body(
    tokens,
    group_choice,
    expert_choice,
    group_weight,
    expert_weight,
    norm_gain,
    w_gate,
    w_up,
    w_down,
):
    count, width = tokens.shape
    half = count // 2
    depth, hidden_width = w_gate.shape[1:]
    chunks, fine = CHUNKS, FINE
    size = half // fine
    items = 4 * fine
    bf16 = jnp.bfloat16
    dma = pltpu.SemaphoreType.DMA
    vmem = pl.BlockSpec(memory_space=pltpu.VMEM)
    hbm = pl.BlockSpec(memory_space=pltpu.HBM)
    return pl.pallas_call(
        functools.partial(layer_kernel, chunks, fine),
        out_shape=jax.ShapeDtypeStruct((count, width), bf16),
        in_specs=[hbm] * 9,
        out_specs=vmem,
        scratch_shapes=[
            pltpu.VMEM((count,), jnp.int32),
            pltpu.VMEM((2, count), jnp.int32),
            pltpu.VMEM((count,), jnp.float32),
            pltpu.VMEM((2, count), jnp.float32),
            pltpu.VMEM((1, norm_gain.shape[0]), jnp.float32),
            pltpu.VMEM((count, width), bf16),
            pltpu.VMEM((1, count), jnp.float32),
            pltpu.VMEM((depth, hidden_width), bf16),
            pltpu.VMEM((depth, hidden_width), bf16),
            pltpu.VMEM(w_down.shape[1:], bf16),
            pltpu.VMEM((items, 4, size, width), bf16),
            pltpu.VMEM((fine, size, width), bf16),
            pltpu.VMEM((4 * chunks, 4, half // chunks, hidden_width), bf16),
            pltpu.VMEM((items, size, width), bf16),
            pltpu.VMEM((items, size, width), bf16),
            pltpu.VMEM((fine, size, width), bf16),
            pltpu.VMEM((2 * fine, count, size), bf16),
            pltpu.VMEM((2 * fine, size, width), bf16),
            pltpu.VMEM((8, count), jnp.float32),
            pltpu.VMEM((2, 8, count), jnp.float32),
            pltpu.VMEM((half // chunks, depth), bf16),
            dma((9,)),
            dma,
            dma((3 * fine,)),
            dma,
            dma((items,)),
            dma((4 * chunks,)),
            dma,
            dma((4 * chunks,)),
            dma((4 * chunks,)),
            dma,
            dma((3 * fine,)),
            dma,
            dma((fine,)),
            dma,
            dma((2,)),
        ],
        compiler_params=pltpu.CompilerParams(
            collective_id=0, has_side_effects=True, vmem_limit_bytes=24 * 1024 * 1024
        ),
    )(
        *[pltpu.with_memory_space_constraint(x, pltpu.HBM) for x in (
        group_choice,
        expert_choice.T,
        group_weight,
        expert_weight.T,
        norm_gain.reshape(1, -1),
        tokens,
        w_gate[0],
        w_up[0],
        w_down[0],
    )])


def pick_body(mesh, *arrays):
    experts = arrays[6].shape[0]
    group_size = min(8, experts // 2)
    choices = arrays[2].shape[1]
    sizes = dict(mesh.shape)
    fits = group_size == choices and experts == 2 * group_size == sizes["ep"]
    fits = fits and sizes["tp"] == sizes["ep"] == len(PROGRAMS)
    fits = fits and arrays[0].shape[0] % (32 * FINE) == 0
    return paired_body if fits else body


def solution(mesh):
    in_specs = (
        P(("grp", "ep"), "tp"),
        P(("grp", "ep")),
        P(("grp", "ep"), None),
        P(("grp", "ep")),
        P(("grp", "ep"), None),
        P(),
        P("ep", None, "tp"),
        P("ep", None, "tp"),
        P("ep", None, "tp"),
    )
    out_specs = P(("grp", "ep"), "tp")

    def layer(*arrays):
        run = jax.shard_map(
            pick_body(mesh, *arrays),
            mesh=mesh,
            in_specs=in_specs,
            out_specs=out_specs,
            check_vma=False,
        )
        return run(*arrays)

    return layer
```
